32 devices in a mesh: sp: 8 (over z, y), tp: 4 (over x, core).
Axes of the slice: x: 2, y: 2, z: 4, core: 2. Of those that a mesh axis runs over, the one named last changes fastest.
Arguments:
- query_one: bfloat16 [2048, 512], P('sp', 'tp'), may hold values from -190 to 190
- query_two: bfloat16 [2048, 512], P('sp', 'tp'), may hold values from -190 to 190
- key_one: bfloat16 [2048, 512], P('sp', 'tp'), may hold values from -10 to 10
- key_two: bfloat16 [2048, 512], P('sp', 'tp'), may hold values from -10 to 10
- values: bfloat16 [2048, 1024], P('sp', 'tp'), may hold values from -6 to 6
- mix_lambda: float32 [8], P('tp'), may hold values from 0.3 to 0.8
- head_gain: float32 [128], replicated, may hold values from 0.1 to 1.9
- stream: bfloat16 [2048, 2048], P('sp', 'tp'), may hold values from -6 to 6
- out_weight: bfloat16 [1024, 2048], P('tp'), may hold values from -0.1875 to 0.1875
- first_gain: float32 [2048], replicated, may hold values from 0.1 to 1.9
- up_weight: bfloat16 [2048, 4096], P('sp', 'tp'), may hold values from -0.125 to 0.125
- down_weight: bfloat16 [4096, 2048], P('tp', 'sp'), may hold values from -0.09375 to 0.09375
- second_gain: float32 [2048], replicated, may hold values from 0.1 to 1.9
Outputs:
- layer_out: bfloat16 [2048, 2048], P(('sp', 'tp'))
The draws below stay inside these ranges and needn't reach their ends.
All inputs are finite; a program needn't handle non-finite values.
Results may differ from the reference program's by a relative error of at most 0.019.
Values may be sent and summed in bfloat16 or wider, within the bound.
A program may use at most 128 MiB of HBM per device.

```python
import math
import jax
import jax.numpy as jnp
from jax import lax

D = 2048
HEADS = 8
QK = 64
VD = 128
FF = 4096
SEQ = 2048
HV = 1024


def drawn_pair(key, which):
    key_query = jax.random.fold_in(key, 11 + which)
    key_keys = jax.random.fold_in(key, 23 + which)
    width = HEADS * QK
    keys_drawn = jnp.clip(jax.random.normal(key_keys, (SEQ, width), jnp.float32), -7.0, 7.0) * 1.3
    queries = jnp.clip(jax.random.normal(key_query, (SEQ, width), jnp.float32), -7.0, 7.0) * 1.3
    return (queries, keys_drawn)


def draw_query_one(key, part):
    return drawn_pair(key, 1)[0].astype(jnp.bfloat16)


def draw_key_one(key, part):
    return drawn_pair(key, 1)[1].astype(jnp.bfloat16)


def draw_query_two(key, part):
    return drawn_pair(key, 2)[0].astype(jnp.bfloat16)


def draw_key_two(key, part):
    return drawn_pair(key, 2)[1].astype(jnp.bfloat16)


def block_scale(rng, dims, split, low, high):
    level, own = 1.0, jax.random.fold_in(rng, 6)
    for dim, blocks in split:
        heights = jnp.exp(jax.random.uniform(jax.random.fold_in(own, dim), (blocks,), jnp.float32, low / len(split), high / len(split)))
        level = level * jnp.repeat(heights, dims[dim] // blocks).reshape([-1 if axis == dim else 1 for axis in range(len(dims))])
    return level


def noise(stream_key, shape, scale, reach, cuts=(), held_as=jnp.bfloat16):
    result = scale * jax.random.normal(stream_key, shape, jnp.float32)
    if cuts:
        result = result * block_scale(stream_key, shape, cuts, -0.22, 0.18)
    return jnp.clip(result, -reach, reach).astype(held_as)


def setup_inputs(seed: int = 0) -> dict:
    key_of = jax.random.split(jax.random.key(seed), 14)
    query_one = draw_query_one(jax.random.fold_in(key_of[13], 71), 0)
    query_two = draw_query_two(jax.random.fold_in(key_of[13], 71), 0)
    key_one = draw_key_one(jax.random.fold_in(key_of[13], 71), 0)
    key_two = draw_key_two(jax.random.fold_in(key_of[13], 71), 0)
    values = noise(key_of[4], (SEQ, HV), 1.0, 6.0, ((0, 8), (1, 4)))
    mix_lambda = jnp.clip(0.3 + 0.5 * jax.random.uniform(key_of[5], (HEADS,), jnp.float32) ** block_scale(key_of[5], (HEADS,), ((0, 4),), -0.2, 0.2), 0.3, 0.8)
    head_gain = jnp.clip(1.0 + 0.18 * jax.random.normal(key_of[6], (VD,), jnp.float32), 0.1, 1.9)
    stream = noise(key_of[7], (SEQ, D), 1.0, 6.0, ((0, 8), (1, 4)))
    out_weight = noise(key_of[8], (HV, D), HV ** -0.5, 0.1875, ((0, 4),))
    first_gain = jnp.clip(1.0 + 0.18 * jax.random.normal(key_of[9], (D,), jnp.float32), 0.1, 1.9)
    up_weight = noise(key_of[10], (D, FF), D ** -0.5, 0.125, ((0, 8), (1, 4)))
    down_weight = noise(key_of[11], (FF, D), FF ** -0.5, 0.09375, ((0, 4), (1, 8)))
    second_gain = jnp.clip(1.0 + 0.18 * jax.random.normal(key_of[12], (D,), jnp.float32), 0.1, 1.9)
    return dict(query_one=query_one, query_two=query_two, key_one=key_one, key_two=key_two, values=values, mix_lambda=mix_lambda, head_gain=head_gain, stream=stream, out_weight=out_weight, first_gain=first_gain, up_weight=up_weight, down_weight=down_weight, second_gain=second_gain)


alpha_mix = 2.0 ** 0.5

def layer_norm(value, gain):
    centre = lax.optimization_barrier(jnp.mean(value, axis=-1, keepdims=True))
    spread = lax.optimization_barrier(jnp.mean(jnp.square(value - centre), axis=-1, keepdims=True))
    return (value - centre) * lax.rsqrt(spread + 1e-05) * gain

def one_map(query_blk, keys, values):
    scores = jnp.dot(query_blk, keys.T, preferred_element_type=jnp.float32) * QK ** (-0.5)
    shifted = scores - lax.optimization_barrier(jnp.max(scores, axis=-1, keepdims=True))
    expo = jnp.exp(shifted)
    total = lax.optimization_barrier(jnp.sum(expo, axis=-1, keepdims=True))
    return jnp.dot(expo.astype(jnp.bfloat16), values, preferred_element_type=jnp.float32) / total

def reference(query_one, query_two, key_one, key_two, values, mix_lambda, head_gain, stream, out_weight, first_gain, up_weight, down_weight, second_gain):

    def heads(array, width):
        return jnp.transpose(array.reshape(SEQ, HEADS, width), (1, 0, 2))
    qblk = math.gcd(SEQ, 512)
    nblk = SEQ // qblk

    def per_head(args):
        q_one, q_two, k_one, k_two, vals, weight = args
        q_one = q_one.reshape(nblk, qblk, QK)
        q_two = q_two.reshape(nblk, qblk, QK)

        def per_block(pair):
            return one_map(pair[0], k_one, vals) - weight * one_map(pair[1], k_two, vals)
        return lax.map(per_block, (q_one, q_two)).reshape(SEQ, VD)
    mixed = lax.map(per_head, (heads(query_one, QK), heads(query_two, QK), heads(key_one, QK), heads(key_two, QK), heads(values, VD), mix_lambda))
    normed = mixed * lax.rsqrt(lax.optimization_barrier(jnp.mean(jnp.square(mixed), axis=-1, keepdims=True)) + 1e-05) * head_gain * 0.8
    attended = jnp.transpose(normed.astype(jnp.bfloat16), (1, 0, 2)).reshape(SEQ, HV)
    pre = alpha_mix * stream.astype(jnp.float32) + jnp.dot(attended, out_weight, preferred_element_type=jnp.float32)
    hidden_in = layer_norm(pre, first_gain).astype(jnp.bfloat16)
    upper = jnp.dot(hidden_in, up_weight, preferred_element_type=jnp.float32)
    act = jnp.square(jax.nn.relu(upper)).astype(jnp.bfloat16)
    post = alpha_mix * hidden_in.astype(jnp.float32) + jnp.dot(act, down_weight, preferred_element_type=jnp.float32)
    return layer_norm(post, second_gain).astype(jnp.bfloat16)
```

```python
import functools
import math

import jax
import jax.numpy as jnp
from jax import lax
from jax.experimental import pallas as pl
from jax.experimental.pallas import tpu as pltpu
from jax.sharding import PartitionSpec as P

MESH = pl.DeviceIdType.MESH
F32, BF16 = jnp.float32, jnp.bfloat16
ALPHA = 2.0**0.5
NT = (((1,), (1,)), ((), ()))
TN = (((0,), (0,)), ((), ()))


def layer_norm(value, gain):
    centre = jnp.mean(value, axis=-1, keepdims=True)
    spread = jnp.mean(jnp.square(value - centre), axis=-1, keepdims=True)
    return (value - centre) * lax.rsqrt(spread + 1e-05) * gain


def kernel(
    nsp, ntp, heads,
    lam_ref, q1_ref, q2_ref, kv_ref, hg_ref, st_ref, ow_ref, g1_ref, up_ref, dn_ref, g2_ref,
    out_ref,
    qm, m_run, l_run, acc, kv_buf, up_buf, dn_buf, ow_buf, st_buf, at_snd, at_buf,
    pre, h_own, h_buf, act, sib_snd, sib_buf, part, red_snd, red_buf,
    loc_sem, kvz, kvy, upz, upy, dnz, dny, owx, ows, sts, ats, hps, hss, sbs, rds,
):
    s, t = lax.axis_index("sp"), lax.axis_index("tp")
    nz, nth = nsp // 2, ntp // 2
    ng = 2 * nth
    z, y = s // 2, s % 2
    zh, zl = z // 2, z % 2
    th, tl = t // 2, t % 2
    sib_t = th * 2 + (1 - tl)
    y_sp = z * 2 + (1 - y)
    grp = zl * nth + th
    tok = q1_ref.shape[0]
    share = tok // ntp
    fh = up_ref.shape[1] // 2
    kw = q1_ref.shape[1]
    qk = kw // heads
    vd = acc.shape[1]
    hv = heads * vd
    d = pre.shape[1]

    def rc(src, dst, sems, i, sp, tp):
        return pltpu.make_async_remote_copy(
            src_ref=src, dst_ref=dst, send_sem=sems.at[0, i], recv_sem=sems.at[1, i],
            device_id={"sp": sp, "tp": tp}, device_id_type=MESH,
        )

    def each(lo, hi, body):
        if hi - lo <= 4:
            for k in range(lo, hi):
                body(k)
        else:
            lax.fori_loop(lo, hi, lambda k, c: (body(k), c)[1], 0)

    def zto(k):
        return lax.rem(z + k, nz)

    def zfrom(k):
        return lax.rem(z + nz - k, nz)

    def kv_z(k):
        return rc(kv_ref, kv_buf.at[s], kvz, k, zto(k) * 2 + y, t)

    def kv_y0():
        return rc(kv_ref, kv_buf.at[s], kvy, 0, y_sp, t)

    def kv_y(k):
        b = zfrom(k) * 2 + y
        return rc(kv_buf.at[b], kv_buf.at[b], kvy, k, y_sp, t)

    def up_half(j):
        return up_ref.at[:, pl.ds(pl.multiple_of(j * fh, fh), fh)]

    def dn_half(j):
        return dn_ref.at[pl.ds(pl.multiple_of(j * fh, fh), fh), :]

    def up_z(k):
        zd = zto(k)
        return rc(up_half(zd % 2), up_buf.at[s], upz, k, zd * 2 + y, t)

    def dn_z(k):
        zd = zto(k)
        return rc(dn_half(zd % 2), dn_buf.at[s], dnz, k, zd * 2 + y, t)

    def up_y0():
        return rc(up_half(zl), up_buf.at[s], upy, 0, y_sp, t)

    def dn_y0():
        return rc(dn_half(zl), dn_buf.at[s], dny, 0, y_sp, t)

    def up_y(k):
        b = zfrom(k) * 2 + y
        return rc(up_buf.at[b], up_buf.at[b], upy, k, y_sp, t)

    def dn_y(k):
        b = zfrom(k) * 2 + y
        return rc(dn_buf.at[b], dn_buf.at[b], dny, k, y_sp, t)

    def ow_x(k):
        return rc(ow_ref, ow_buf.at[t], owx, k, s, lax.rem(th + k, nth) * 2 + tl)

    def ow_s0():
        return rc(ow_ref, ow_buf.at[t], ows, 0, s, sib_t)

    def ow_s(k):
        b = lax.rem(th + nth - k, nth) * 2 + tl
        return rc(ow_buf.at[b], ow_buf.at[b], ows, k, s, sib_t)

    def rows_of(tt):
        return pl.ds(pl.multiple_of(tt * share, share), share)

    def st_c(k):
        td = lax.rem(t + k, ntp)
        return rc(st_ref.at[rows_of(td), :], st_buf.at[t], sts, k, s, td)

    def at_c(k):
        td = lax.rem(t + k, ntp)
        return rc(at_snd.at[rows_of(td), :], at_buf.at[t], ats, k, s, td)

    def grp_dev(g):
        return (zh * 2 + g // nth) * 2 + y, lax.rem(g, nth) * 2 + tl

    def h_p(k):
        sp, tp = grp_dev(lax.rem(grp + k, ng))
        return rc(h_own, h_buf.at[tl, grp], hps, k, sp, tp)

    def h_s0():
        return rc(h_own, h_buf.at[tl, grp], hss, 0, s, sib_t)

    def h_s(k):
        g = lax.rem(grp + ng - k, ng)
        return rc(h_buf.at[tl, g], h_buf.at[tl, g], hss, k, s, sib_t)

    def sib_c():
        return rc(sib_snd, sib_buf, sbs, 0, s, sib_t)

    def red_c(k):
        g = lax.rem(grp + k, ng)
        sp, tp = grp_dev(g)
        return rc(red_snd.at[g], red_buf.at[grp], rds, k, sp, tp)

    barrier = pltpu.get_barrier_semaphore()

    def greet(sp, tp):
        pl.semaphore_signal(barrier, inc=1, device_id={"sp": sp, "tp": tp}, device_id_type=MESH)

    each(1, nz, lambda k: greet(zto(k) * 2 + y, t))
    greet(y_sp, t)
    each(1, ntp, lambda k: greet(s, lax.rem(t + k, ntp)))
    each(1, nth, lambda k: greet((zh * 2 + 1 - zl) * 2 + y, lax.rem(th + k, nth) * 2 + tl))
    pl.semaphore_wait(barrier, (nz - 1) + 1 + (ntp - 1) + (nth - 1))

    each(1, nz, lambda k: kv_z(k).start())
    kv_y0().start()
    each(1, ntp, lambda k: st_c(k).start())
    each(1, nth, lambda k: ow_x(k).start())
    ow_s0().start()
    locals_ = [
        pltpu.make_async_copy(ow_ref, ow_buf.at[t], loc_sem.at[0]),
        pltpu.make_async_copy(up_half(zl), up_buf.at[s], loc_sem.at[1]),
        pltpu.make_async_copy(dn_half(zl), dn_buf.at[s], loc_sem.at[2]),
    ]
    for c in locals_:
        c.start()
    each(1, nz, lambda k: up_z(k).start())
    each(1, nz, lambda k: dn_z(k).start())

    scale = qk ** (-0.5)
    lane = lax.broadcasted_iota(jnp.int32, (tok, kw), 1)
    for i, q_ref in enumerate((q1_ref, q2_ref)):
        qv = q_ref[...].astype(F32) * scale
        for h in range(heads):
            keep = (lane >= h * qk) & (lane < (h + 1) * qk)
            qm[i * heads + h] = jnp.where(keep, qv, 0.0).astype(BF16)
    m_run[...] = jnp.full(m_run.shape, -1e30, F32)
    l_run[...] = jnp.zeros(l_run.shape, F32)
    acc[...] = jnp.zeros(acc.shape, F32)

    def absorb(block):
        for h in range(heads):
            v = block[:, 2 * kw + h * vd : 2 * kw + (h + 1) * vd]
            for i in range(2):
                r = i * heads + h
                sc = lax.dot_general(
                    block[:, i * kw : (i + 1) * kw], qm[r], NT, preferred_element_type=F32
                )
                old = m_run[r]
                new = jnp.maximum(old, jnp.max(sc, axis=0, keepdims=True))
                fac = jnp.exp(old - new)
                ex = jnp.exp(sc - new)
                l_run[r] = l_run[r] * fac + jnp.sum(ex, axis=0, keepdims=True)
                acc[r] = acc[r] * fac + lax.dot_general(
                    v, ex.astype(BF16), TN, preferred_element_type=F32
                )
                m_run[r] = new

    absorb(kv_ref)

    def z_step(k, c):
        kv_z(k).wait_recv()
        kv_y(k).start()
        absorb(kv_buf.at[zfrom(k) * 2 + y])
        return c

    lax.fori_loop(1, nz, z_step, 0)
    up_y0().start()
    dn_y0().start()

    def y_step(k, c):
        kv_y(k).wait_recv()
        absorb(kv_buf.at[zfrom(k) * 2 + 1 - y])
        return c

    lax.fori_loop(0, nz, y_step, 0)

    for k in range(1, nth):
        ow_x(k).wait_recv()
        ow_s(k).start()

    for h in range(heads):
        mixed = acc[h] / l_run[h] - lam_ref[h] * (acc[heads + h] / l_run[heads + h])
        inv = lax.rsqrt(jnp.mean(jnp.square(mixed), axis=0, keepdims=True) + 1e-05)
        normed = jnp.transpose(mixed * inv) * hg_ref[...] * 0.8
        at_snd[:, h * vd : (h + 1) * vd] = normed.astype(BF16)
    each(1, ntp, lambda k: at_c(k).start())
    at_buf[t] = at_snd[rows_of(t), :]
    st_buf[t] = st_ref[rows_of(t), :]
    up_z(1).wait_recv()
    up_y(1).start()

    each(1, ntp, lambda k: st_c(k).wait_recv())
    cols = st_ref.shape[1]
    for b in range(ntp):
        pre[:, b * cols : (b + 1) * cols] = ALPHA * st_buf[b].astype(F32)
    locals_[0].wait()
    ow_s0().wait_recv()
    for k in range(1, nth):
        ow_s(k).wait_recv()
    each(1, ntp, lambda k: at_c(k).wait_recv())
    for b in range(ntp):
        pre[...] += jnp.dot(at_buf[b], ow_buf[b], preferred_element_type=F32)
    h_own[...] = layer_norm(pre[...], g1_ref[...]).astype(BF16)
    each(1, ng, lambda k: h_p(k).start())
    h_s0().start()
    h_buf[tl, grp] = h_own[...]

    def up_fwd(k):
        up_z(k).wait_recv()
        up_y(k).start()

    each(2, nz, up_fwd)

    def h_fwd(k):
        h_p(k).wait_recv()
        h_s(k).start()

    each(1, ng, h_fwd)

    def dn_fwd(k):
        dn_z(k).wait_recv()
        dn_y(k).start()

    each(1, nz, dn_fwd)
    h_s0().wait_recv()
    each(1, ng, lambda k: h_s(k).wait_recv())
    locals_[1].wait()
    up_y0().wait_recv()
    each(1, nz, lambda k: up_y(k).wait_recv())

    half = ng * share
    depth = up_buf.shape[1]
    for side in range(2):
        for c in range(2 if fh % 256 == 0 else 1):
            wide = fh // (2 if fh % 256 == 0 else 1)
            at = slice(c * wide, (c + 1) * wide)
            hid = h_buf[side].reshape(half, d)
            w = up_buf[:, :, at].reshape(d, wide)
            up = jnp.dot(hid, w, preferred_element_type=F32)
            act[side, :, at] = jnp.square(jnp.maximum(up, 0.0)).astype(BF16)

    locals_[2].wait()
    dn_y0().wait_recv()
    each(1, nz, lambda k: dn_y(k).wait_recv())
    out_w = dn_buf.shape[2]
    for b in range(nsp):
        at = slice(b * out_w, (b + 1) * out_w)
        res = jnp.dot(act[1 - tl], dn_buf[b], preferred_element_type=F32)
        sib_snd[:, at] = res.astype(BF16)
    sib_c().start()
    for b in range(nsp):
        at = slice(b * out_w, (b + 1) * out_w)
        part[:, at] = jnp.dot(act[tl], dn_buf[b], preferred_element_type=F32)
    sib_c().wait_recv()

    def red_step(k):
        g = lax.rem(grp + k, ng)
        rows = pl.ds(pl.multiple_of(g * share, share), share)
        red_snd[g] = (part[rows, :] + sib_buf[rows, :].astype(F32)).astype(BF16)
        red_c(k).start()

    for k in range(ng - 1, 0, -1):
        red_step(k)
    rows = pl.ds(pl.multiple_of(grp * share, share), share)
    pre[...] = part[rows, :] + sib_buf[rows, :].astype(F32) + ALPHA * h_own[...].astype(F32)
    for k in range(ng - 1, 0, -1):
        red_c(k).wait_recv()
        pre[...] += red_buf[lax.rem(grp + ng - k, ng)].astype(F32)
    out_ref[...] = layer_norm(pre[...], g2_ref[...]).astype(BF16)

    kv_y0().wait_send()
    up_y0().wait_send()
    dn_y0().wait_send()
    ow_s0().wait_send()
    h_s0().wait_send()
    sib_c().wait_send()
    for first, last, fns in (
        (1, nz, (kv_z, kv_y, up_z, up_y, dn_z, dn_y)),
        (1, nth, (ow_x, ow_s)),
        (1, ntp, (st_c, at_c)),
        (1, ng, (h_p, h_s, red_c)),
    ):
        each(first, last, lambda k: [f(k).wait_send() for f in fns])


def local(nsp, ntp, q1, q2, k1, k2, vals, lam, hg, stream, ow, g1, up, dn, g2):
    tok = q1.shape[0]
    heads = lam.shape[0]
    hv = vals.shape[1]
    vd = hv // heads
    d = ow.shape[1]
    nz, nth = nsp // 2, ntp // 2
    ng = 2 * nth
    share = tok // ntp
    fh = up.shape[1] // 2
    kv = jnp.concatenate([k1, k2, vals], axis=1)
    vm = pl.BlockSpec(memory_space=pltpu.VMEM)
    anys = pl.BlockSpec(memory_space=pl.ANY)
    sem = lambda n: pltpu.SemaphoreType.DMA((2, n))
    return pl.pallas_call(
        functools.partial(kernel, nsp, ntp, heads),
        out_shape=jax.ShapeDtypeStruct((share, d), BF16),
        in_specs=[pl.BlockSpec(memory_space=pltpu.SMEM), vm, vm, vm, vm, vm, anys, vm, anys, anys, vm],
        out_specs=vm,
        scratch_shapes=[
            pltpu.VMEM((2 * heads, tok, q1.shape[1]), BF16),
            pltpu.VMEM((2 * heads, 1, tok), F32),
            pltpu.VMEM((2 * heads, 1, tok), F32),
            pltpu.VMEM((2 * heads, vd, tok), F32),
            pltpu.VMEM((nsp,) + kv.shape, BF16),
            pltpu.VMEM((nsp, up.shape[0], fh), BF16),
            pltpu.VMEM((nsp, fh, dn.shape[1]), BF16),
            pltpu.VMEM((ntp,) + ow.shape, BF16),
            pltpu.VMEM((ntp, share, stream.shape[1]), BF16),
            pltpu.VMEM((tok, hv), BF16),
            pltpu.VMEM((ntp, share, hv), BF16),
            pltpu.VMEM((share, d), F32),
            pltpu.VMEM((share, d), BF16),
            pltpu.VMEM((2, ng, share, d), BF16),
            pltpu.VMEM((2, ng * share, fh), BF16),
            pltpu.VMEM((ng * share, d), BF16),
            pltpu.VMEM((ng * share, d), BF16),
            pltpu.VMEM((ng * share, d), F32),
            pltpu.VMEM((ng, share, d), BF16),
            pltpu.VMEM((ng, share, d), BF16),
            pltpu.SemaphoreType.DMA((3,)),
            sem(nz), sem(nz), sem(nz), sem(nz), sem(nz), sem(nz),
            sem(nth), sem(nth), sem(ntp), sem(ntp), sem(ng), sem(ng), sem(1), sem(ng),
        ],
        compiler_params=pltpu.CompilerParams(
            collective_id=0, has_side_effects=True, vmem_limit_bytes=60 * 1024 * 1024
        ),
    )(lam, q1, q2, kv, hg.reshape(1, vd), stream, ow, g1.reshape(1, d), up, dn, g2.reshape(1, d))


def solution(mesh):
    in_specs = (
        P("sp", "tp"),
        P("sp", "tp"),
        P("sp", "tp"),
        P("sp", "tp"),
        P("sp", "tp"),
        P("tp"),
        P(),
        P("sp", "tp"),
        P("tp", None),
        P(),
        P("sp", "tp"),
        P("tp", "sp"),
        P(),
    )
    body = functools.partial(local, mesh.shape["sp"], mesh.shape["tp"])
    return jax.shard_map(
        body, mesh=mesh, in_specs=in_specs, out_specs=P(("sp", "tp"), None), check_vma=False
    )
```

```python
import functools
import math

import jax
import jax.numpy as jnp
from jax import lax
from jax.experimental import pallas as pl
from jax.experimental.pallas import tpu as pltpu
from jax.sharding import PartitionSpec as P

MESH = pl.DeviceIdType.MESH
F32, BF16 = jnp.float32, jnp.bfloat16
ALPHA = 2.0**0.5
NT = (((1,), (1,)), ((), ()))
TN = (((0,), (0,)), ((), ()))


def layer_norm(value, gain):
    centre = jnp.mean(value, axis=-1, keepdims=True)
    spread = jnp.mean(jnp.square(value - centre), axis=-1, keepdims=True)
    return (value - centre) * lax.rsqrt(spread + 1e-05) * gain


def kernel(
    nsp, ntp, heads,
    lam_ref, qkv_ref, hg_ref, st_ref, ow_ref, g1_ref, up_ref, dn_ref, g2_ref,
    out_ref,
    lam_all, q_buf, qm, m_run, l_run, acc, kv_buf, up_buf, dn_buf, ow_buf, st_buf, at_snd, at_buf,
    pre, h_own, h_buf, act, sib_snd, sib_buf, part, red_snd, red_buf,
    loc_sem, lms, qs, kvz, kvy, kvs, upz, upy, dnz, dny, owx, ows, sts, ats, hps, hss, sbs, rds,
):
    s, t = lax.axis_index("sp"), lax.axis_index("tp")
    nz, nth = nsp // 2, ntp // 2
    ng = 2 * nth
    z, y = s // 2, s % 2
    zh, zl = z // 2, z % 2
    th, tl = t // 2, t % 2
    sib_t = th * 2 + (1 - tl)
    y_sp = z * 2 + (1 - y)
    grp = zl * nth + th
    tok = qkv_ref.shape[1]
    share = tok // ntp
    fh = up_ref.shape[1] // 2
    vd = acc.shape[1]
    qw = q_buf.shape[2]
    qk = qw // 2
    tall = q_buf.shape[1]
    nzb = q_buf.shape[0]
    d = pre.shape[1]
    zq = lax.rem(z, nzb)
    zb = z - zq
    entry_t, head_j = zq // heads, lax.rem(zq, heads)
    entry = tl == entry_t
    head = th * nzb + zq

    def rc(src, dst, sems, i, sp, tp, arrive=None):
        arrive = i if arrive is None else arrive
        return pltpu.make_async_remote_copy(
            src_ref=src, dst_ref=dst, send_sem=sems.at[0, i], recv_sem=sems.at[1, arrive],
            device_id={"sp": sp, "tp": tp}, device_id_type=MESH,
        )

    def each(lo, hi, body):
        if hi - lo <= 4:
            for k in range(lo, hi):
                body(k)
        else:
            lax.fori_loop(lo, hi, lambda k, c: (body(k), c)[1], 0)

    def zto(k):
        return lax.rem(z + k, nz)

    def zfrom(k):
        return lax.rem(z + nz - k, nz)

    def slab(j):
        return qkv_ref.at[j, :, pl.ds(qw, qw + vd)]

    def q_c(j, hf):
        zd = zb + heads * tl + j
        return rc(
            qkv_ref.at[j, pl.ds(hf * tall, tall), pl.ds(0, qw)], q_buf.at[zq],
            qs, j * 2 + hf, zd * 2 + y, th * 2 + hf, zq,
        )

    def q_in(i):
        return rc(q_buf.at[i], q_buf.at[i], qs, 0, y_sp, t, i)

    def kv_z(j, r):
        zd = r * nzb + heads * tl + j
        return rc(
            slab(j), kv_buf.at[s], kvz, r * heads + j, zd * 2 + y, t, lax.rem(zd - z + nz, nz)
        )

    def kv_zin(k):
        b = zfrom(k) * 2 + y
        return rc(kv_buf.at[b], kv_buf.at[b], kvz, 0, y_sp, t, k)

    def kv_y(k):
        b = zfrom(k) * 2 + y
        return rc(kv_buf.at[b], kv_buf.at[b], kvy, k, y_sp, t)

    def kv_y0():
        return rc(slab(head_j), kv_buf.at[s], kvy, 0, y_sp, t)

    def kv_s(k, side):
        b = zfrom(k) * 2 + lax.rem(y + side, 2)
        return rc(kv_buf.at[b], kv_buf.at[b], kvs, side * nz + k, s, sib_t)

    def kv_s0():
        return rc(slab(head_j), kv_buf.at[s], kvs, 0, s, sib_t)

    def up_half(j):
        return up_ref.at[:, pl.ds(pl.multiple_of(j * fh, fh), fh)]

    def dn_half(j):
        return dn_ref.at[pl.ds(pl.multiple_of(j * fh, fh), fh), :]

    def up_z(k):
        zd = zto(k)
        return rc(up_half(zd % 2), up_buf.at[s], upz, k, zd * 2 + y, t)

    def dn_z(k):
        zd = zto(k)
        return rc(dn_half(zd % 2), dn_buf.at[s], dnz, k, zd * 2 + y, t)

    def up_y0():
        return rc(up_half(zl), up_buf.at[s], upy, 0, y_sp, t)

    def dn_y0():
        return rc(dn_half(zl), dn_buf.at[s], dny, 0, y_sp, t)

    def up_y(k):
        b = zfrom(k) * 2 + y
        return rc(up_buf.at[b], up_buf.at[b], upy, k, y_sp, t)

    def dn_y(k):
        b = zfrom(k) * 2 + y
        return rc(dn_buf.at[b], dn_buf.at[b], dny, k, y_sp, t)

    def ow_x(k):
        return rc(ow_ref, ow_buf.at[t], owx, k, s, lax.rem(th + k, nth) * 2 + tl)

    def ow_s0():
        return rc(ow_ref, ow_buf.at[t], ows, 0, s, sib_t)

    def ow_s(k):
        b = lax.rem(th + nth - k, nth) * 2 + tl
        return rc(ow_buf.at[b], ow_buf.at[b], ows, k, s, sib_t)

    def rows_of(tt):
        return pl.ds(pl.multiple_of(tt * share, share), share)

    def st_c(k):
        td = lax.rem(t + k, ntp)
        return rc(st_ref.at[rows_of(td), :], st_buf.at[t], sts, k, s, td)

    def at_c(i, u):
        rows = pl.ds(i * tall + u * share, share)
        cols = pl.ds(pl.multiple_of(head * vd, vd), vd)
        return rc(
            at_snd.at[rows, :], at_buf.at[:, cols], ats, i * nth + u,
            (zb + i) * 2 + y, tl * nth + u, head,
        )

    def at_in(hd):
        ref = at_buf.at[:, pl.ds(hd * vd, vd)]
        return rc(ref, ref, ats, 0, y_sp, t, hd)

    mine = t // nth == tl

    def at_self(hd):
        return mine & (head == hd)

    def grp_dev(g):
        return (zh * 2 + g // nth) * 2 + y, lax.rem(g, nth) * 2 + tl

    def h_p(k):
        sp, tp = grp_dev(lax.rem(grp + k, ng))
        return rc(h_own, h_buf.at[tl, grp], hps, k, sp, tp)

    def h_s0():
        return rc(h_own, h_buf.at[tl, grp], hss, 0, s, sib_t)

    def h_s(k):
        g = lax.rem(grp + ng - k, ng)
        return rc(h_buf.at[tl, g], h_buf.at[tl, g], hss, k, s, sib_t)

    def sib_c():
        return rc(sib_snd, sib_buf, sbs, 0, s, sib_t)

    def red_c(k):
        g = lax.rem(grp + k, ng)
        sp, tp = grp_dev(g)
        return rc(red_snd.at[g], red_buf.at[grp], rds, k, sp, tp)

    barrier = pltpu.get_barrier_semaphore()

    def greet(sp, tp):
        pl.semaphore_signal(barrier, inc=1, device_id={"sp": sp, "tp": tp}, device_id_type=MESH)

    for i in range(nzb):
        for tt in range(ntp):
            pl.when((i != zq) | (tt != t))(functools.partial(greet, (zb + i) * 2 + y, tt))
    if nz > nzb:
        each(0, nz, lambda k: pl.when((k < zb) | (k >= zb + nzb))(lambda: greet(k * 2 + y, t)))
    greet(y_sp, t)
    pl.semaphore_wait(barrier, nzb * ntp - 1 + nz - nzb + 1)

    def q_self(j, hf):
        return (zq == heads * tl + j) & (hf == tl)

    pairs = [(j, hf) for j in range(heads) for hf in range(2)]
    for j, hf in pairs:
        pl.when(jnp.logical_not(q_self(j, hf)))(lambda: q_c(j, hf).start())

        @pl.when(q_self(j, hf))
        def _():
            q_buf[zq] = qkv_ref[j, hf * tall : (hf + 1) * tall, :qw]

    def lam_c():
        return rc(lam_ref, lam_all.at[tl], lms, 0, s, sib_t)

    lam_all[tl] = lam_ref[...]

    def kv_out(fn):
        for j in range(heads):
            each(0, nz // nzb, lambda r: pl.when(r * nzb + heads * tl + j != z)(lambda: fn(kv_z(j, r))))

    kv_out(lambda c: c.start())

    @pl.when(entry)
    def _():
        kv_y0().start()
        kv_s0().start()
        kv_buf[s] = qkv_ref[head_j, :, qw:]

    lam_c().start()
    each(1, ntp, lambda k: st_c(k).start())
    each(1, nth, lambda k: ow_x(k).start())
    ow_s0().start()
    locals_ = [
        pltpu.make_async_copy(ow_ref, ow_buf.at[t], loc_sem.at[0]),
        pltpu.make_async_copy(up_half(zl), up_buf.at[s], loc_sem.at[1]),
        pltpu.make_async_copy(dn_half(zl), dn_buf.at[s], loc_sem.at[2]),
    ]
    for c in locals_:
        c.start()
    each(1, nz, lambda k: up_z(k).start())

    scale = qk ** (-0.5)
    m_run[...] = jnp.full(m_run.shape, -1e30, F32)
    l_run[...] = jnp.zeros(l_run.shape, F32)
    acc[...] = jnp.zeros(acc.shape, F32)
    lane = lax.broadcasted_iota(jnp.int32, (tall, qw), 1)
    for i in range(nzb):
        pl.when(jnp.logical_not((zq == i) & entry))(lambda: q_in(i).wait_recv())
        qv = q_buf[i].astype(F32) * scale
        for mp in range(2):
            keep = (lane >= mp * qk) & (lane < (mp + 1) * qk)
            qm[mp, i * tall : (i + 1) * tall, :] = jnp.where(keep, qv, 0.0).astype(BF16)

    def absorb(block):
        v = block[:, qw:]
        for r in range(2):
            sc = lax.dot_general(block[:, :qw], qm[r], NT, preferred_element_type=F32)
            old = m_run[r]
            new = jnp.maximum(old, jnp.max(sc, axis=0, keepdims=True))
            fac = jnp.exp(old - new)
            ex = jnp.exp(sc - new)
            l_run[r] = l_run[r] * fac + jnp.sum(ex, axis=0, keepdims=True)
            acc[r] = acc[r] * fac + lax.dot_general(
                v, ex.astype(BF16), TN, preferred_element_type=F32
            )
            m_run[r] = new

    def own_step():
        pl.when(jnp.logical_not(entry))(lambda: kv_s0().wait_recv())
        absorb(kv_buf.at[s])

    own_step()

    def z_step(k, c):
        @pl.when(entry)
        def _():
            kv_zin(k).wait_recv()
            kv_y(k).start()
            kv_s(k, 0).start()

        pl.when(jnp.logical_not(entry))(lambda: kv_s(k, 0).wait_recv())
        absorb(kv_buf.at[zfrom(k) * 2 + y])
        return c

    lax.fori_loop(1, nz, z_step, 0)
    up_y0().start()
    dn_y0().start()

    def y_step(k, c):
        @pl.when(entry)
        def _():
            kv_y(k).wait_recv()
            kv_s(k, 1).start()

        pl.when(jnp.logical_not(entry))(lambda: kv_s(k, 1).wait_recv())
        absorb(kv_buf.at[zfrom(k) * 2 + 1 - y])
        return c

    lax.fori_loop(0, nz, y_step, 0)
    up_z(1).wait_recv()
    up_y(1).start()

    for k in range(1, nth):
        ow_x(k).wait_recv()
        ow_s(k).start()

    lam_c().wait_recv()
    lam = lam_all[entry_t, head_j][:, :1]
    mixed = acc[0] / l_run[0] - lam * (acc[1] / l_run[1])
    inv = lax.rsqrt(jnp.mean(jnp.square(mixed), axis=0, keepdims=True) + 1e-05)
    normed = jnp.transpose(mixed * inv) * hg_ref[...] * 0.8
    at_snd[...] = normed.astype(BF16)
    spots = [(i, u) for i in range(nzb) for u in range(nth)]
    for i, u in spots:
        own = (zq == i) & (tl * nth + u == t)
        pl.when(jnp.logical_not(own))(lambda: at_c(i, u).start())

        @pl.when(own)
        def _():
            cols = pl.ds(pl.multiple_of(head * vd, vd), vd)
            at_buf[:, cols] = at_snd[i * tall + u * share : i * tall + (u + 1) * share, :]

    st_buf[t] = st_ref[rows_of(t), :]
    up_z(2).wait_recv()
    up_y(2).start()

    each(1, ntp, lambda k: st_c(k).wait_recv())
    cols = st_ref.shape[1]
    for b in range(ntp):
        pre[:, b * cols : (b + 1) * cols] = ALPHA * st_buf[b].astype(F32)
    locals_[0].wait()
    ow_s0().wait_recv()
    for k in range(1, nth):
        ow_s(k).wait_recv()
    for hd in range(nzb * nth):
        pl.when(jnp.logical_not(at_self(hd)))(lambda: at_in(hd).wait_recv())
    for b in range(ntp):
        at = slice(b * cols, (b + 1) * cols)
        full = ow_buf[:, :, at].reshape(at_buf.shape[1], cols)
        pre[:, at] += jnp.dot(at_buf[...], full, preferred_element_type=F32)
    h_own[...] = layer_norm(pre[...], g1_ref[...]).astype(BF16)
    each(1, ng, lambda k: h_p(k).start())
    h_s0().start()
    each(1, nz, lambda k: dn_z(k).start())
    h_buf[tl, grp] = h_own[...]

    def up_fwd(k):
        up_z(k).wait_recv()
        up_y(k).start()

    each(3, nz, up_fwd)

    def h_fwd(k):
        h_p(k).wait_recv()
        h_s(k).start()

    def dn_fwd(k):
        dn_z(k).wait_recv()
        dn_y(k).start()

    each(1, ng, h_fwd)
    dn_fwd(1)
    h_s0().wait_recv()
    each(1, ng, lambda k: h_s(k).wait_recv())
    locals_[1].wait()
    up_y0().wait_recv()
    each(1, nz, lambda k: up_y(k).wait_recv())

    half = ng * share
    depth = up_buf.shape[1]
    for side in range(2):
        for c in range(2 if fh % 256 == 0 else 1):
            wide = fh // (2 if fh % 256 == 0 else 1)
            at = slice(c * wide, (c + 1) * wide)
            hid = h_buf[side].reshape(half, d)
            w = up_buf[:, :, at].reshape(d, wide)
            up = jnp.dot(hid, w, preferred_element_type=F32)
            act[side, :, at] = jnp.square(jnp.maximum(up, 0.0)).astype(BF16)

    each(2, nz, dn_fwd)
    locals_[2].wait()
    dn_y0().wait_recv()
    each(1, nz, lambda k: dn_y(k).wait_recv())
    out_w = dn_buf.shape[2]
    for b in range(nsp):
        at = slice(b * out_w, (b + 1) * out_w)
        res = jnp.dot(act[1 - tl], dn_buf[b], preferred_element_type=F32)
        sib_snd[:, at] = res.astype(BF16)
    sib_c().start()
    for b in range(nsp):
        at = slice(b * out_w, (b + 1) * out_w)
        part[:, at] = jnp.dot(act[tl], dn_buf[b], preferred_element_type=F32)
    sib_c().wait_recv()

    def red_step(k):
        g = lax.rem(grp + k, ng)
        rows = pl.ds(pl.multiple_of(g * share, share), share)
        red_snd[g] = (part[rows, :] + sib_buf[rows, :].astype(F32)).astype(BF16)
        red_c(k).start()

    for k in range(ng - 1, 0, -1):
        red_step(k)
    rows = pl.ds(pl.multiple_of(grp * share, share), share)
    pre[...] = part[rows, :] + sib_buf[rows, :].astype(F32) + ALPHA * h_own[...].astype(F32)
    for k in range(ng - 1, 0, -1):
        red_c(k).wait_recv()
        pre[...] += red_buf[lax.rem(grp + ng - k, ng)].astype(F32)
    out_ref[...] = layer_norm(pre[...], g2_ref[...]).astype(BF16)

    for j, hf in pairs:
        pl.when(jnp.logical_not(q_self(j, hf)))(lambda: q_c(j, hf).wait_send())
    for i, u in spots:
        own = (zq == i) & (tl * nth + u == t)
        pl.when(jnp.logical_not(own))(lambda: at_c(i, u).wait_send())
    kv_out(lambda c: c.wait_send())

    @pl.when(entry)
    def _():
        kv_y0().wait_send()
        kv_s0().wait_send()
        each(1, nz, lambda k: kv_y(k).wait_send())
        each(1, nz, lambda k: kv_s(k, 0).wait_send())
        each(0, nz, lambda k: kv_s(k, 1).wait_send())

    lam_c().wait_send()
    up_y0().wait_send()
    dn_y0().wait_send()
    ow_s0().wait_send()
    h_s0().wait_send()
    sib_c().wait_send()
    for first, last, fns in (
        (1, nz, (up_z, up_y, dn_z, dn_y)),
        (1, nth, (ow_x, ow_s)),
        (1, ntp, (st_c,)),
        (1, ng, (h_p, h_s, red_c)),
    ):
        each(first, last, lambda k: [f(k).wait_send() for f in fns])


def local(nsp, ntp, q1, q2, k1, k2, vals, lam, hg, stream, ow, g1, up, dn, g2):
    tok = q1.shape[0]
    heads = lam.shape[0]
    hv = vals.shape[1]
    vd = hv // heads
    d = ow.shape[1]
    nz, nth = nsp // 2, ntp // 2
    ng = 2 * nth
    share = tok // ntp
    fh = up.shape[1] // 2
    qk = q1.shape[1] // heads
    parts = [a.reshape(tok, heads, -1) for a in (q1, q2, k1, k2, vals)]
    qkv = jnp.concatenate(parts, axis=2).transpose(1, 0, 2)
    nzb, tall = 2 * heads, nth * share
    lam = jnp.broadcast_to(lam[:, None, None], (heads, 1, 128))
    vm = pl.BlockSpec(memory_space=pltpu.VMEM)
    anys = pl.BlockSpec(memory_space=pl.ANY)
    sem = lambda n: pltpu.SemaphoreType.DMA((2, n))
    return pl.pallas_call(
        functools.partial(kernel, nsp, ntp, heads),
        out_shape=jax.ShapeDtypeStruct((share, d), BF16),
        in_specs=[vm, vm, vm, vm, anys, vm, anys, anys, vm],
        out_specs=vm,
        scratch_shapes=[
            pltpu.VMEM((2,) + lam.shape, F32),
            pltpu.VMEM((nzb, tall, 2 * qk), BF16),
            pltpu.VMEM((2, nzb * tall, 2 * qk), BF16),
            pltpu.VMEM((2, 1, nzb * tall), F32),
            pltpu.VMEM((2, 1, nzb * tall), F32),
            pltpu.VMEM((2, vd, nzb * tall), F32),
            pltpu.VMEM((nsp, tok, 2 * qk + vd), BF16),
            pltpu.VMEM((nsp, up.shape[0], fh), BF16),
            pltpu.VMEM((nsp, fh, dn.shape[1]), BF16),
            pltpu.VMEM((ntp,) + ow.shape, BF16),
            pltpu.VMEM((ntp, share, stream.shape[1]), BF16),
            pltpu.VMEM((nzb * tall, vd), BF16),
            pltpu.VMEM((share, ntp * hv), BF16),
            pltpu.VMEM((share, d), F32),
            pltpu.VMEM((share, d), BF16),
            pltpu.VMEM((2, ng, share, d), BF16),
            pltpu.VMEM((2, ng * share, fh), BF16),
            pltpu.VMEM((ng * share, d), BF16),
            pltpu.VMEM((ng * share, d), BF16),
            pltpu.VMEM((ng * share, d), F32),
            pltpu.VMEM((ng, share, d), BF16),
            pltpu.VMEM((ng, share, d), BF16),
            pltpu.SemaphoreType.DMA((3,)),
            sem(1),
            sem(max(2 * heads, nzb)), sem(nz), sem(nz), sem(2 * nz), sem(nz), sem(nz), sem(nz), sem(nz),
            sem(nth), sem(nth), sem(ntp), sem(max(nzb * nth, nzb * nth)), sem(ng), sem(ng), sem(1), sem(ng),
        ],
        compiler_params=pltpu.CompilerParams(
            collective_id=0, has_side_effects=True, vmem_limit_bytes=60 * 1024 * 1024
        ),
    )(lam, qkv, hg.reshape(1, vd), stream, ow, g1.reshape(1, d), up, dn, g2.reshape(1, d))


def solution(mesh):
    in_specs = (
        P("sp", "tp"),
        P("sp", "tp"),
        P("sp", "tp"),
        P("sp", "tp"),
        P("sp", "tp"),
        P("tp"),
        P(),
        P("sp", "tp"),
        P("tp", None),
        P(),
        P("sp", "tp"),
        P("tp", "sp"),
        P(),
    )
    body = functools.partial(local, mesh.shape["sp"], mesh.shape["tp"])
    return jax.shard_map(
        body, mesh=mesh, in_specs=in_specs, out_specs=P(("sp", "tp"), None), check_vma=False
    )
```
